32 devices in a mesh: ep: 4 (over y, x), tp: 8 (over z, core).
Axes of the slice: x: 2, y: 2, z: 4, core: 2. Of those that a mesh axis runs over, the one named last changes fastest.
Arguments:
- tokens: bfloat16 [64, 2048], P('ep'), may hold values from -6 to 6
- routes: int32 [64, 4], P('ep'), may hold values from 0 to 7, all different within a row; in each aligned block of 16 rows (0 to 15, 16 to 31, ...) at most 16 rows name the same one
- route_weight: float32 [64, 4], P('ep'), may hold values from 0.2 to 1
- mixer_gain: float32 [2048], replicated, may hold values from 0.1 to 1.9
- gate_weight: bfloat16 [2048, 4096], P(None, 'tp'), may hold values from -0.125 to 0.125
- input_weight: bfloat16 [2048, 4096], P(None, 'tp'), may hold values from -0.125 to 0.125
- step_weight: bfloat16 [2048, 64], P(None, 'tp'), may hold values from -0.125 to 0.125
- write_weight: bfloat16 [2048, 512], P('tp'), may hold values from -0.125 to 0.125
- read_weight: bfloat16 [2048, 512], P('tp'), may hold values from -0.125 to 0.125
- step_bias: float32 [64], P('tp'), may hold values from -3 to 0.5
- decay_log: float32 [64], P('tp'), may hold values from -2 to 0.5
- decay_jolt: float32 [64, 64], P('ep', 'tp'), may hold values from -1 to 0
- filter_taps: bfloat16 [4, 4096], P(None, 'tp'), may hold values from -3 to 3
- filter_state: bfloat16 [64, 3, 4096], P('ep', None, 'tp'), may hold values from -6 to 6
- scan_state: float32 [64, 64, 64, 128], P('ep', 'tp'), may hold values from -2 to 2
- skip_gain: float32 [64], P('tp'), may hold values from 0.5 to 2
- head_gain: float32 [4096], P('tp'), may hold values from 0.1 to 1.9
- output_weight: bfloat16 [4096, 2048], P('tp'), may hold values from -0.09375 to 0.09375
- channel_gain: float32 [2048], replicated, may hold values from 0.1 to 1.9
- expert_gate: bfloat16 [8, 2048, 2048], P('ep', None, 'tp'), may hold values from -0.125 to 0.125
- expert_up: bfloat16 [8, 2048, 2048], P('ep', None, 'tp'), may hold values from -0.125 to 0.125
- expert_down: bfloat16 [8, 2048, 2048], P('ep', 'tp'), may hold values from -0.125 to 0.125
- shared_gate: bfloat16 [2048, 2048], P(None, 'tp'), may hold values from -0.125 to 0.125
- shared_up: bfloat16 [2048, 2048], P(None, 'tp'), may hold values from -0.125 to 0.125
- shared_down: bfloat16 [2048, 2048], P('tp'), may hold values from -0.125 to 0.125
Outputs:
- layer_out: bfloat16 [64, 2048], P('ep', 'tp')
- new_state: float32 [64, 64, 64, 128], P('ep', 'tp')
- new_filter: bfloat16 [64, 3, 4096], P('ep', None, 'tp')
The draws below stay inside these ranges and needn't reach their ends.
Inputs may be any that keep to these rules, and one draw needn't show every extreme that they name: `routes`: each row names 4 different experts. In each aligned block of 16 rows (the rows of one index of ep) no expert is named by more than 16 rows, a bound that some block reaches.
All inputs are finite; a program needn't handle non-finite values.
Results may differ from the reference program's by a relative error of at most 0.025.
Values may be sent and summed in bfloat16 or wider, within the bound.
A program may use at most 64 MiB of HBM per device.

```python
import math
import jax
import jax.numpy as jnp
import numpy as np
from jax import lax

D = 2048
HEADS = 64
HEAD_DIM = 64
DI = 4096
GROUPS = 4
STATE = 128
CONV = 4
FF_E = 2048
FF_S = 2048
TOPK = 4
SEQ_DEV = 16
SEQS = 64
EXPERTS = 8
CAP = 16
N_EP = 4
N_TP = 8


def levels(own_key, dims, split, low, largest):
    gain = 1.0
    for dim, blocks in split:
        steps = jax.random.uniform(jax.random.fold_in(jax.random.fold_in(own_key, 6), dim), (blocks,), jnp.float32, low / len(split), largest / len(split))
        gain = gain * jnp.repeat(jnp.exp(steps), dims[dim] // blocks).reshape((-1,) + (1,) * (len(dims) - 1 - dim))
    return gain


def routed_block(stream_key, own, number, rows, count, top, reach, slope):
    ranking = jax.random.permutation(stream_key, count)
    crowded, ordinary = portions_of(count, rows * top, reach, slope, True), portions_of(count, rows * top, reach, slope, False)
    places = jnp.arange(count)

    def named(tallies, offset_by):
        used = int((tallies > 0).sum())
        fixed = max(1, used // 4)
        moved = fixed + (places - fixed + offset_by * (used - fixed)) % max(1, count - fixed)
        return jnp.zeros((count,), jnp.int32).at[ranking[jnp.where(places < fixed, places, moved)]].set(jnp.asarray(tallies, jnp.int32))

    tallies = jnp.where(number % 4 == 0, named(crowded, number // 4), named(ordinary, number - number // 4 - 1))
    mixed = jax.random.permutation(jax.random.fold_in(own, 3), count)
    donor, taker = mixed[0:count // 2 * 2:2], mixed[1:count // 2 * 2:2]
    margin = jnp.minimum(tallies[donor] - 1, reach - tallies[taker]) // 2
    margin = jnp.where((donor == ranking[0]) | (taker == ranking[0]) | (tallies[taker] == 0), 0, jnp.maximum(margin, 0))
    moved = jax.random.randint(jax.random.fold_in(own, 4), (count // 2,), 0, 1 << 20) % (margin + 1)
    tallies = tallies.at[donor].add(-moved).at[taker].add(moved)
    items = jnp.searchsorted(jnp.cumsum(tallies), jnp.arange(rows * top), side="right").astype(jnp.int32)
    grid = items.reshape(top, rows).T
    grid = grid[jax.random.permutation(jax.random.fold_in(own, 1), rows)]
    offset_by = jax.random.randint(jax.random.fold_in(own, 2), (rows, 1), 0, top)
    return jnp.take_along_axis(grid, (jnp.arange(top)[None, :] + offset_by) % top, axis=1)


def portions_of(amount, total, limit, skew, full):
    loads = [(1 << 20) // math.isqrt(grade ** skew) + 1 for grade in range(1, amount + 1)]
    largest = limit if full else min(limit, max(-(-total // amount), total * loads[0] // sum(loads)))
    least = 1 if total - largest >= amount - 1 else 0
    counts, spare = [largest] + [least] * (amount - 1), total - largest - least * (amount - 1)
    while spare > 0:
        movable = [i for i in range(1, amount) if counts[i] < largest] or [i for i in range(1, amount) if counts[i] < limit]
        mass, left = sum([loads[i] for i in movable]), spare
        for i in movable:
            more = min(limit - counts[i], max(1, left * loads[i] // mass), spare)
            counts[i] = counts[i] + more
            spare = spare - more
    return np.array(counts)


def bell_draw(stream_key, extent, scale, reach, shards=(), kind=jnp.bfloat16):
    level = levels(stream_key, extent, shards, -0.22, 0.18) if shards else 1.0
    drawn = jax.random.normal(stream_key, extent, jnp.float32) * scale * level
    return jnp.minimum(jnp.maximum(drawn, -reach), reach).astype(kind)


def setup_inputs(seed: int = 0) -> dict:
    arg_keys = jax.random.split(jax.random.key(seed), 26)
    tokens = bell_draw(arg_keys[0], (SEQS, D), 1.0, 6.0, ((0, 4),))
    routes_keys = jax.random.split(jax.random.fold_in(arg_keys[1], 1), SEQS // SEQ_DEV)
    routes_turns = jax.random.permutation(jax.random.fold_in(arg_keys[1], 3), SEQS // SEQ_DEV)
    routes = jax.vmap(lambda own, number: routed_block(jax.random.fold_in(arg_keys[1], 2), own, number, SEQ_DEV, EXPERTS, TOPK, CAP, 2))(routes_keys, routes_turns).reshape((SEQS, TOPK))
    route_weight = jnp.clip(jnp.exp(math.log(1.0) - 1.609438 * jax.random.uniform(arg_keys[2], (SEQS, TOPK), jnp.float32) ** levels(arg_keys[2], (SEQS, TOPK), ((0, 4),), -0.2, 0.2)), 0.2, 1.0)
    mixer_gain = jnp.clip(1.0 + 0.18 * jax.random.normal(arg_keys[3], (D,), jnp.float32), 0.1, 1.9)
    gate_weight = bell_draw(arg_keys[4], (D, DI), D ** -0.5, 0.125, ((1, 8),))
    input_weight = bell_draw(arg_keys[5], (D, DI), D ** -0.5, 0.125, ((1, 8),))
    step_weight = bell_draw(arg_keys[6], (D, HEADS), D ** -0.5, 0.125, ((1, 8),))
    write_weight = bell_draw(arg_keys[7], (D, GROUPS * STATE), D ** -0.5, 0.125, ((0, 8),))
    read_weight = bell_draw(arg_keys[8], (D, GROUPS * STATE), D ** -0.5, 0.125, ((0, 8),))
    step_bias = jnp.clip(-3.0 + 3.5 * jax.random.uniform(arg_keys[9], (HEADS,), jnp.float32) ** levels(arg_keys[9], (HEADS,), ((0, 8),), -0.2, 0.2), -3.0, 0.5)
    decay_log = jnp.clip(-2.0 + 2.5 * jax.random.uniform(arg_keys[10], (HEADS,), jnp.float32) ** levels(arg_keys[10], (HEADS,), ((0, 8),), -0.2, 0.2), -2.0, 0.5)
    decay_jolt = jnp.clip(-1.0 + 1.0 * jax.random.uniform(arg_keys[11], (SEQS, HEADS), jnp.float32) ** levels(arg_keys[11], (SEQS, HEADS), ((0, 4), (1, 8)), -0.2, 0.2), -1.0, 0.0)
    filter_taps = bell_draw(arg_keys[12], (CONV, DI), 0.5, 3.0, ((1, 8),))
    filter_state = bell_draw(arg_keys[13], (SEQS, CONV - 1, DI), 1.0, 6.0, ((0, 4), (2, 8)))
    scan_state = bell_draw(arg_keys[14], (SEQS, HEADS, HEAD_DIM, STATE), 0.3, 2.0, ((0, 4), (1, 8)), jnp.float32)
    skip_gain = jnp.clip(jnp.exp(math.log(2.0) - 1.3862944 * jax.random.uniform(arg_keys[15], (HEADS,), jnp.float32) ** levels(arg_keys[15], (HEADS,), ((0, 8),), -0.2, 0.2)), 0.5, 2.0)
    head_gain = jnp.clip(1.0 + 0.18 * jax.random.normal(arg_keys[16], (DI,), jnp.float32), 0.1, 1.9)
    output_weight = bell_draw(arg_keys[17], (DI, D), DI ** -0.5, 0.09375, ((0, 8),))
    channel_gain = jnp.clip(1.0 + 0.18 * jax.random.normal(arg_keys[18], (D,), jnp.float32), 0.1, 1.9)
    expert_gate = bell_draw(arg_keys[19], (EXPERTS, D, FF_E), D ** -0.5, 0.125, ((0, 4), (2, 8)))
    expert_up = bell_draw(arg_keys[20], (EXPERTS, D, FF_E), D ** -0.5, 0.125, ((0, 4), (2, 8)))
    expert_down = bell_draw(arg_keys[21], (EXPERTS, FF_E, D), FF_E ** -0.5, 0.125, ((0, 4), (1, 8)))
    shared_gate = bell_draw(arg_keys[22], (D, FF_S), D ** -0.5, 0.125, ((1, 8),))
    shared_up = bell_draw(arg_keys[23], (D, FF_S), D ** -0.5, 0.125, ((1, 8),))
    shared_down = bell_draw(arg_keys[24], (FF_S, D), FF_S ** -0.5, 0.125, ((0, 8),))
    return {"tokens": tokens, "routes": routes, "route_weight": route_weight, "mixer_gain": mixer_gain, "gate_weight": gate_weight, "input_weight": input_weight, "step_weight": step_weight, "write_weight": write_weight, "read_weight": read_weight, "step_bias": step_bias, "decay_log": decay_log, "decay_jolt": decay_jolt, "filter_taps": filter_taps, "filter_state": filter_state, "scan_state": scan_state, "skip_gain": skip_gain, "head_gain": head_gain, "output_weight": output_weight, "channel_gain": channel_gain, "expert_gate": expert_gate, "expert_up": expert_up, "expert_down": expert_down, "shared_gate": shared_gate, "shared_up": shared_up, "shared_down": shared_down}


EPS = 1e-06

def rms_normed(values, scaling):
    mean_square = lax.optimization_barrier(jnp.mean(values * values, axis=-1, keepdims=True))
    return values * lax.rsqrt(mean_square + EPS) * scaling

def route_targets(route_ids, experts, capacity):
    count_rows, top_picks = route_ids.shape
    flattened = route_ids.reshape(count_rows * top_picks).astype(jnp.int32)
    onehot = (flattened[:, None] == jnp.arange(experts, dtype=jnp.int32)[None, :]).astype(jnp.int32)
    before = jnp.cumsum(onehot, axis=0) - onehot
    slot_index = lax.optimization_barrier(jnp.sum(before * onehot, axis=1))
    return (flattened * capacity + slot_index).astype(jnp.int32).reshape(count_rows, top_picks)

def shard_rounded(hidden, weight):
    count_rows = hidden.shape[0]
    slice_width = hidden.shape[1] // N_TP
    hidden_parts = hidden.reshape(count_rows, N_TP, slice_width).astype(jnp.float32)
    weight_parts = weight.reshape(N_TP, slice_width, weight.shape[1]).astype(jnp.float32)
    partial_sums = jnp.einsum('rtf,tfd->rtd', hidden_parts, weight_parts).astype(jnp.bfloat16)
    partial_sums = lax.optimization_barrier(partial_sums)
    return lax.optimization_barrier(jnp.sum(partial_sums.astype(jnp.float32), axis=1))

def reference(tokens, routes, route_weight, mixer_gain, gate_weight, input_weight, step_weight, write_weight, read_weight, step_bias, decay_log, decay_jolt, filter_taps, filter_state, scan_state, skip_gain, head_gain, output_weight, channel_gain, expert_gate, expert_up, expert_down, shared_gate, shared_up, shared_down):
    tokens_f = tokens.astype(jnp.float32)
    normed = rms_normed(tokens_f, mixer_gain).astype(jnp.bfloat16)
    write_in = jnp.dot(normed, write_weight, preferred_element_type=jnp.float32)
    read_in = jnp.dot(normed, read_weight, preferred_element_type=jnp.float32)
    gate_rows = jnp.dot(normed, gate_weight, preferred_element_type=jnp.float32).astype(jnp.bfloat16)
    input_rows = jnp.dot(normed, input_weight, preferred_element_type=jnp.float32).astype(jnp.bfloat16)
    step_raw = jnp.dot(normed, step_weight, preferred_element_type=jnp.float32)
    seq_count = tokens.shape[0]
    per_group = HEADS // GROUPS
    write_vec = jnp.repeat(jax.nn.silu(write_in).reshape(seq_count, GROUPS, STATE), per_group, axis=1)
    read_vec = jnp.repeat(jax.nn.silu(read_in).reshape(seq_count, GROUPS, STATE), per_group, axis=1)
    window = jnp.concatenate([filter_state, input_rows[:, None, :]], axis=1)
    filtered = jax.nn.silu(lax.optimization_barrier(jnp.sum(window.astype(jnp.float32) * filter_taps.astype(jnp.float32)[None], axis=1)))
    step_size = jax.nn.softplus(step_raw + step_bias)
    log_decay = decay_jolt - jnp.exp(decay_log) * step_size
    head_input = filtered.reshape(seq_count, HEADS, HEAD_DIM)
    new_state = jnp.exp(log_decay)[:, :, None, None] * scan_state + (step_size[:, :, None] * head_input)[:, :, :, None] * write_vec[:, :, None, :]
    readout = jnp.einsum('shpn,shn->shp', new_state, read_vec, precision=lax.Precision.HIGHEST)
    readout = readout + skip_gain[None, :, None] * head_input
    gate_heads = gate_rows.astype(jnp.float32).reshape(seq_count, HEADS, HEAD_DIM)
    gated = rms_normed(readout * jax.nn.silu(gate_heads), head_gain.reshape(HEADS, HEAD_DIM))
    gated = gated.astype(jnp.bfloat16).reshape(seq_count, HEADS * HEAD_DIM)
    mixed = jnp.dot(gated, output_weight, preferred_element_type=jnp.float32).astype(jnp.bfloat16)
    resid = (tokens_f + mixed.astype(jnp.float32)).astype(jnp.bfloat16)
    normed_ffn = rms_normed(resid.astype(jnp.float32), channel_gain).astype(jnp.bfloat16)
    shared_hidden = (jax.nn.silu(jnp.dot(normed_ffn, shared_gate, preferred_element_type=jnp.float32)) * jnp.dot(normed_ffn, shared_up, preferred_element_type=jnp.float32)).astype(jnp.bfloat16)
    shared_out = shard_rounded(shared_hidden, shared_down)
    targets = jax.vmap(lambda block: route_targets(block, EXPERTS, CAP))(routes.reshape(N_EP, SEQ_DEV, TOPK))
    block_index = jnp.arange(N_EP, dtype=jnp.int32)[:, None, None]
    expert_index = targets // CAP
    slot_index = targets % CAP
    position = ((expert_index * N_EP + block_index) * CAP + slot_index).reshape(-1).astype(jnp.int32)
    token_index = jnp.broadcast_to(jnp.arange(seq_count, dtype=jnp.int32).reshape(N_EP, SEQ_DEV, 1), targets.shape).reshape(-1)
    row_token = jnp.full((EXPERTS * N_EP * CAP,), seq_count, jnp.int32).at[position].set(token_index)
    padded = jnp.concatenate([normed_ffn, jnp.zeros((1, D), jnp.bfloat16)], axis=0)

    def one_expert(operands):
        token_ids, gate_part, up_part, down_part = operands
        chosen = padded[token_ids]
        hidden = (jax.nn.silu(jnp.dot(chosen, gate_part, preferred_element_type=jnp.float32)) * jnp.dot(chosen, up_part, preferred_element_type=jnp.float32)).astype(jnp.bfloat16)
        return shard_rounded(hidden, down_part).astype(jnp.bfloat16)
    expert_out = lax.map(one_expert, (row_token.reshape(EXPERTS, N_EP * CAP), expert_gate, expert_up, expert_down))
    picked = expert_out.reshape(EXPERTS * N_EP * CAP, D)[position].reshape(seq_count, TOPK, D)
    routed = lax.optimization_barrier(jnp.sum(route_weight[:, :, None] * picked.astype(jnp.float32), axis=1))
    layer_out = (resid.astype(jnp.float32) + shared_out + routed).astype(jnp.bfloat16)
    return (layer_out, new_state, window[:, 1:, :])
```

```python
import functools

import jax
import jax.numpy as jnp
from jax import lax
from jax.experimental import pallas as pl
from jax.experimental.pallas import tpu as pltpu
from jax.sharding import PartitionSpec as P

HEADS = 64
HEAD_DIM = 64
GROUPS = 4
STATE = 128

EPS = 1e-06
F32 = jnp.float32
BF16 = jnp.bfloat16
MESH = pl.DeviceIdType.MESH
VMEM_LIMIT = 56 * 1024 * 1024


def dot(a, b):
    return jnp.dot(a, b, preferred_element_type=F32)


def dot_nt(a, b):
    return lax.dot_general(a, b, (((1,), (1,)), ((), ())), preferred_element_type=F32)


def split(v):
    high = v.astype(BF16)
    return high, (v - high.astype(F32)).astype(BF16)


def softplus(v):
    return jnp.maximum(v, 0.0) + jnp.log1p(jnp.exp(-jnp.abs(v)))


def project_kernel(
    n_tp,
    heads_here,
    tokens_ref,
    gain_ref,
    step_ref,
    gate_hbm,
    input_hbm,
    write_hbm,
    read_hbm,
    vec_ref,
    gate_ref,
    input_ref,
    raw_ref,
    gate_buf,
    input_buf,
    write_buf,
    read_buf,
    normed_buf,
    out_buf,
    in_buf,
    load_sem,
    send_sem,
    recv_sem,
):
    ep = lax.axis_index("ep")
    tp = lax.axis_index("tp")
    loads = [
        pltpu.make_async_copy(src, dst, load_sem.at[i])
        for i, (src, dst) in enumerate(
            (
                (write_hbm, write_buf),
                (read_hbm, read_buf),
                (input_hbm, input_buf),
                (gate_hbm, gate_buf),
            )
        )
    ]
    for load in loads:
        load.start()
    barrier = pltpu.get_barrier_semaphore()

    def greet(k, carry):
        pl.semaphore_signal(
            barrier, inc=1, device_id=(ep, lax.rem(tp + k, n_tp)), device_id_type=MESH
        )
        return carry

    lax.fori_loop(1, n_tp, greet, 0)
    tokens = tokens_ref[...].astype(F32)
    scale = lax.rsqrt(jnp.mean(tokens * tokens, axis=-1, keepdims=True) + EPS)
    normed_buf[...] = (tokens * scale * gain_ref[...]).astype(BF16)
    features = write_buf.shape[0]
    own = normed_buf[:, pl.ds(pl.multiple_of(tp * features, features), features)]
    loads[0].wait()
    loads[1].wait()
    write_part = dot(own, write_buf[...]).astype(BF16)
    read_part = dot(own, read_buf[...]).astype(BF16)
    for g in range(GROUPS):
        out_buf[g, :, :STATE] = write_part[:, g * STATE : (g + 1) * STATE]
        out_buf[g, :, STATE:] = read_part[:, g * STATE : (g + 1) * STATE]
    per_group = HEADS // GROUPS
    pl.semaphore_wait(barrier, n_tp - 1)

    def copy_to(k):
        peer = lax.rem(tp + k, n_tp)
        return pltpu.make_async_remote_copy(
            src_ref=out_buf.at[(peer * heads_here) // per_group],
            dst_ref=in_buf.at[tp],
            send_sem=send_sem.at[peer],
            recv_sem=recv_sem.at[tp],
            device_id=(ep, peer),
            device_id_type=MESH,
        )

    def copy_from(k):
        peer = lax.rem(tp + k, n_tp)
        return pltpu.make_async_remote_copy(
            src_ref=out_buf.at[0],
            dst_ref=in_buf.at[peer],
            send_sem=send_sem.at[peer],
            recv_sem=recv_sem.at[peer],
            device_id=(ep, peer),
            device_id_type=MESH,
        )

    def send(k, carry):
        copy_to(k).start()
        return carry

    lax.fori_loop(1, n_tp, send, 0)
    in_buf[tp] = out_buf[(tp * heads_here) // per_group]
    normed = normed_buf[...]
    raw_ref[...] = dot_nt(step_ref[...], normed)
    loads[2].wait()
    input_ref[...] = dot(normed, input_buf[...]).astype(BF16)
    loads[3].wait()
    gate_ref[...] = dot(normed, gate_buf[...]).astype(BF16)

    def receive(k, carry):
        copy_from(k).wait_recv()
        return carry

    lax.fori_loop(1, n_tp, receive, 0)
    vec_ref[...] = jax.nn.silu(jnp.sum(in_buf[...].astype(F32), axis=0))

    def sent(k, carry):
        copy_to(k).wait_send()
        return carry

    lax.fori_loop(1, n_tp, sent, 0)


def state_kernel(
    bias_ref,
    rate_ref,
    skip_ref,
    vec_ref,
    gate_ref,
    input_ref,
    raw_ref,
    jolt_ref,
    taps_ref,
    filter_ref,
    gain_ref,
    state_hbm,
    weight_hbm,
    part_ref,
    new_hbm,
    new_filter_ref,
    state_buf,
    new_buf,
    weight_buf,
    decay_buf,
    x_buf,
    read_buf,
    load_sem,
    store_sem,
    weight_sem,
):
    rows, width, _ = state_buf.shape
    heads = jolt_ref.shape[0]
    for s in range(rows):
        pltpu.make_async_copy(state_hbm.at[s], state_buf.at[s], load_sem.at[s]).start()
    weight_load = pltpu.make_async_copy(weight_hbm, weight_buf, weight_sem)
    weight_load.start()
    taps = taps_ref[...].astype(F32)
    last = filter_ref.shape[0]
    inputs = input_ref[...]
    total = inputs.astype(F32) * taps[last : last + 1]
    for i in range(last):
        total = total + filter_ref[i].astype(F32) * taps[i : i + 1]
        new_filter_ref[i] = filter_ref[i + 1] if i + 1 < last else inputs
    filtered = jax.nn.silu(total)
    pad = jnp.zeros((128 - rows, width), F32)
    filtered_t = jnp.transpose(jnp.concatenate([filtered, pad], axis=0))[:, :rows]
    head_ids = lax.broadcasted_iota(jnp.int32, (heads, rows), 0)
    bias = jnp.zeros((heads, rows), F32)
    rate = jnp.zeros((heads, rows), F32)
    for h in range(heads):
        bias = jnp.where(head_ids == h, bias_ref[h], bias)
        rate = jnp.where(head_ids == h, rate_ref[h], rate)
    step = softplus(raw_ref[...] + bias)
    decay = jnp.exp(jolt_ref[...] - jnp.exp(rate) * step)

    def expand(v):
        return jnp.concatenate(
            [jnp.broadcast_to(v[h : h + 1], (HEAD_DIM, rows)) for h in range(heads)], axis=0
        )

    decay_buf[...] = expand(decay)
    x_buf[...] = expand(step) * filtered_t
    for s in range(rows):
        pltpu.make_async_copy(state_hbm.at[s], state_buf.at[s], load_sem.at[s]).wait()
        write = vec_ref[s : s + 1, :STATE]
        new = decay_buf[:, s : s + 1] * state_buf[s] + x_buf[:, s : s + 1] * write
        new_buf[s] = new
        pltpu.make_async_copy(new_buf.at[s], new_hbm.at[s], store_sem.at[s]).start()
        read_high, read_low = split(vec_ref[s : s + 1, STATE:])
        high, low = split(new)
        read_buf[s : s + 1, :] = (
            dot_nt(read_high, high) + dot_nt(read_low, high) + dot_nt(read_high, low)
        )
    lane_head = lax.broadcasted_iota(jnp.int32, (1, width), 1) // HEAD_DIM
    skip = jnp.zeros((1, width), F32)
    for h in range(heads):
        skip = jnp.where(lane_head == h, skip_ref[h], skip)
    value = (read_buf[...] + skip * filtered) * jax.nn.silu(gate_ref[...].astype(F32))
    same = (
        lax.broadcasted_iota(jnp.int32, (width, width), 0) // HEAD_DIM
        == lax.broadcasted_iota(jnp.int32, (width, width), 1) // HEAD_DIM
    )
    block = jnp.where(same, 1.0, 0.0).astype(BF16)
    high, low = split(value * value)
    mean_square = (dot(high, block) + dot(low, block)) * (1.0 / HEAD_DIM)
    gated = (value * lax.rsqrt(mean_square + EPS) * gain_ref[...]).astype(BF16)
    weight_load.wait()
    columns = part_ref.shape[2]
    for t in range(part_ref.shape[0]):
        part_ref[t] = dot(gated, weight_buf[:, t * columns : (t + 1) * columns]).astype(BF16)
    for s in range(rows):
        pltpu.make_async_copy(new_buf.at[s], new_hbm.at[s], store_sem.at[s]).wait()


def expert_kernel(
    n_ep,
    n_tp,
    part_ref,
    tokens_ref,
    routes_ref,
    route_weight_ref,
    gain_ref,
    gate_hbm,
    up_hbm,
    down_hbm,
    sgate_hbm,
    sup_hbm,
    sdown_hbm,
    out_ref,
    gate_buf,
    up_buf,
    down_buf,
    sgate_buf,
    sup_buf,
    sdown_buf,
    mix_buf,
    resid_buf,
    share_buf,
    normed_buf,
    total_buf,
    term_buf,
    back_buf,
    load_sem,
    mix_send,
    mix_recv,
    share_send,
    share_recv,
    resid_send,
    resid_recv,
    back_send,
    back_recv,
):
    ep = lax.axis_index("ep")
    tp = lax.axis_index("tp")
    me = ep * n_tp + tp
    n_all = n_ep * n_tp
    rows, columns = out_ref.shape
    loads = [
        pltpu.make_async_copy(src, dst, load_sem.at[i])
        for i, (src, dst) in enumerate(
            (
                (sgate_hbm, sgate_buf),
                (sup_hbm, sup_buf),
                (gate_hbm, gate_buf),
                (up_hbm, up_buf),
                (sdown_hbm, sdown_buf),
                (down_hbm, down_buf),
            )
        )
    ]
    barrier = pltpu.get_barrier_semaphore()

    def place(k):
        other = lax.rem(me + k, n_all)
        return other // n_tp, lax.rem(other, n_tp)

    def loop(low, high, act):
        def body(k, carry):
            act(k)
            return carry

        lax.fori_loop(low, high, body, 0)

    loop(
        1,
        n_all,
        lambda k: pl.semaphore_signal(barrier, inc=1, device_id=place(k), device_id_type=MESH),
    )
    for load in loads:
        load.start()

    lanes = share_buf.shape[2]
    lane_ids = lax.broadcasted_iota(jnp.int32, (rows, lanes), 1)
    share = jnp.zeros((rows, lanes), F32)
    for k in range(routes_ref.shape[1]):
        share = share + jnp.where(
            routes_ref[:, k : k + 1] == lane_ids, route_weight_ref[:, k : k + 1], 0.0
        )
    share_buf[ep] = share

    def mix_copy(k, slot):
        peer = lax.rem(tp + k, n_tp)
        return pltpu.make_async_remote_copy(
            src_ref=part_ref.at[peer],
            dst_ref=mix_buf.at[tp if slot is None else peer],
            send_sem=mix_send.at[peer],
            recv_sem=mix_recv.at[tp if slot is None else peer],
            device_id=(ep, peer),
            device_id_type=MESH,
        )

    def share_copy(k, slot):
        peer = lax.rem(ep + k, n_ep)
        mine = ep if slot is None else peer
        return pltpu.make_async_remote_copy(
            src_ref=share_buf.at[mine],
            dst_ref=share_buf.at[mine],
            send_sem=share_send.at[peer],
            recv_sem=share_recv.at[mine],
            device_id=(peer, tp),
            device_id_type=MESH,
        )

    def resid_copy(k, slot):
        e, t = place(k)
        at_e, at_t = (ep, tp) if slot is None else (e, t)
        return pltpu.make_async_remote_copy(
            src_ref=resid_buf.at[at_e, at_t],
            dst_ref=resid_buf.at[at_e, at_t],
            send_sem=resid_send.at[e * n_tp + t],
            recv_sem=resid_recv.at[at_e * n_tp + at_t],
            device_id=(e, t),
            device_id_type=MESH,
        )

    def back_copy(e, t, slot):
        at_e, at_t = (ep, tp) if slot is None else (e, t)
        return pltpu.make_async_remote_copy(
            src_ref=term_buf.at[t, e],
            dst_ref=back_buf.at[at_e * n_tp + at_t],
            send_sem=back_send.at[e * n_tp + t],
            recv_sem=back_recv.at[at_e * n_tp + at_t],
            device_id=(e, t),
            device_id_type=MESH,
        )

    pl.semaphore_wait(barrier, n_all - 1)
    loop(1, n_tp, lambda k: mix_copy(k, None).start())
    loop(1, n_ep, lambda k: share_copy(k, None).start())
    mix_buf[tp] = part_ref[tp]
    own_tokens = tokens_ref[:, pl.ds(pl.multiple_of(tp * columns, columns), columns)]
    loop(1, n_tp, lambda k: mix_copy(k, 1).wait_recv())
    mixed = jnp.sum(mix_buf[...].astype(F32), axis=0).astype(BF16)
    resid_own = (own_tokens.astype(F32) + mixed.astype(F32)).astype(BF16)
    resid_buf[ep, tp] = resid_own
    loop(1, n_all, lambda k: resid_copy(k, None).start())

    def normalise(e):
        square = jnp.zeros((rows, columns), F32)
        for t in range(n_tp):
            value = resid_buf[e, t].astype(F32)
            square = square + value * value
        mean_square = jnp.sum(square, axis=-1, keepdims=True) * (1.0 / (n_tp * columns))
        scale = lax.rsqrt(mean_square + EPS)
        for t in range(n_tp):
            at = slice(t * columns, (t + 1) * columns)
            value = resid_buf[e, t].astype(F32) * scale * gain_ref[:, at]
            normed_buf[pl.ds(pl.multiple_of(e * rows, rows), rows), at] = value.astype(BF16)

    loop(
        0, n_all - 1, lambda k: resid_copy(k + 1, 1).wait_recv()
    )
    loop(0, n_ep, normalise)
    normed_own = normed_buf[pl.ds(pl.multiple_of(ep * rows, rows), rows), :]
    loads[0].wait()
    loads[1].wait()
    shared_hidden = (
        jax.nn.silu(dot(normed_own, sgate_buf[...])) * dot(normed_own, sup_buf[...])
    ).astype(BF16)
    loads[2].wait()
    loads[3].wait()
    hidden = []
    for j in range(gate_buf.shape[0]):
        normed = normed_buf[...]
        hidden.append(
            (jax.nn.silu(dot(normed, gate_buf[j])) * dot(normed, up_buf[j])).astype(BF16)
        )
    loop(1, n_ep, lambda k: share_copy(k, 1).wait_recv())
    shares = share_buf[...].reshape(n_ep * rows, lanes)
    all_lanes = lax.broadcasted_iota(jnp.int32, shares.shape, 1)
    local = gate_buf.shape[0]
    scales = [
        jnp.sum(jnp.where(all_lanes == ep * local + j, shares, 0.0), axis=1, keepdims=True)
        for j in range(local)
    ]
    loads[4].wait()
    loads[5].wait()
    for t in range(n_tp):
        at = slice(t * columns, (t + 1) * columns)
        term = scales[0] * dot(hidden[0], down_buf[0, :, at])
        for j in range(1, local):
            term = term + scales[j] * dot(hidden[j], down_buf[j, :, at])
        total_buf[t] = term.reshape(n_ep, rows, columns)
        total_buf[t, ep] = total_buf[t, ep] + dot(shared_hidden, sdown_buf[:, at])
        term_buf[t] = total_buf[t].astype(BF16)

        def give(e):
            @pl.when(e * n_tp + t != me)
            def _():
                back_copy(e, t, None).start()

        loop(0, n_ep, give)
    back_buf[me] = term_buf[tp, ep]

    def others(act):
        def body(k):
            e, t = place(k)
            act(e, t)

        loop(1, n_all, body)

    others(lambda e, t: back_copy(e, t, 1).wait_recv())
    out_ref[...] = (
        resid_buf[ep, tp].astype(F32) + jnp.sum(back_buf[...].astype(F32), axis=0)
    ).astype(BF16)
    loop(1, n_tp, lambda k: mix_copy(k, None).wait_send())
    loop(1, n_ep, lambda k: share_copy(k, None).wait_send())
    loop(1, n_all, lambda k: resid_copy(k, None).wait_send())
    others(lambda e, t: back_copy(e, t, None).wait_send())


def on_device(
    tokens,
    routes,
    route_weight,
    mixer_gain,
    gate_weight,
    input_weight,
    step_weight,
    write_weight,
    read_weight,
    step_bias,
    decay_log,
    decay_jolt,
    filter_taps,
    filter_state,
    scan_state,
    skip_gain,
    head_gain,
    output_weight,
    channel_gain,
    expert_gate,
    expert_up,
    expert_down,
    shared_gate,
    shared_up,
    shared_down,
):
    rows, model = tokens.shape
    n_tp = lax.axis_size("tp")
    n_ep = lax.axis_size("ep")
    n_all = n_tp * n_ep
    columns = model // n_tp
    heads_here = step_bias.shape[0]
    width = gate_weight.shape[1]
    vmem = pl.BlockSpec(memory_space=pltpu.VMEM)
    smem = pl.BlockSpec(memory_space=pltpu.SMEM)
    hbm = pl.BlockSpec(memory_space=pl.ANY)
    dma = pltpu.SemaphoreType.DMA
    shape = jax.ShapeDtypeStruct

    vecs, gate_rows, input_rows, step_raw = pl.pallas_call(
        functools.partial(project_kernel, n_tp, heads_here),
        out_shape=(
            shape((rows, 2 * STATE), F32),
            shape((rows, width), BF16),
            shape((rows, width), BF16),
            shape((heads_here, rows), F32),
        ),
        in_specs=[vmem] * 3 + [hbm] * 4,
        out_specs=(vmem,) * 4,
        scratch_shapes=[
            pltpu.VMEM(gate_weight.shape, BF16),
            pltpu.VMEM(input_weight.shape, BF16),
            pltpu.VMEM(write_weight.shape, BF16),
            pltpu.VMEM(read_weight.shape, BF16),
            pltpu.VMEM((rows, model), BF16),
            pltpu.VMEM((GROUPS, rows, 2 * STATE), BF16),
            pltpu.VMEM((n_tp, rows, 2 * STATE), BF16),
            dma((4,)),
            dma((n_tp,)),
            dma((n_tp,)),
        ],
        compiler_params=pltpu.CompilerParams(
            collective_id=0, has_side_effects=True, vmem_limit_bytes=VMEM_LIMIT
        ),
        name="project",
    )(
        tokens,
        mixer_gain.reshape(1, model),
        step_weight.T,
        gate_weight,
        input_weight,
        write_weight,
        read_weight,
    )

    taps = filter_state.shape[1]
    part, new_state, new_filter = pl.pallas_call(
        state_kernel,
        out_shape=(
            shape((n_tp, rows, columns), BF16),
            shape((rows, width, STATE), F32),
            shape((taps, rows, width), BF16),
        ),
        in_specs=[smem] * 3 + [vmem] * 8 + [hbm] * 2,
        out_specs=(vmem, hbm, vmem),
        scratch_shapes=[
            pltpu.VMEM((rows, width, STATE), F32),
            pltpu.VMEM((rows, width, STATE), F32),
            pltpu.VMEM(output_weight.shape, BF16),
            pltpu.VMEM((width, rows), F32),
            pltpu.VMEM((width, rows), F32),
            pltpu.VMEM((rows, width), F32),
            dma((rows,)),
            dma((rows,)),
            dma,
        ],
        compiler_params=pltpu.CompilerParams(vmem_limit_bytes=VMEM_LIMIT),
        name="state",
    )(
        step_bias,
        decay_log,
        skip_gain,
        vecs,
        gate_rows,
        input_rows,
        step_raw,
        decay_jolt.T,
        filter_taps,
        jnp.transpose(filter_state, (1, 0, 2)),
        head_gain.reshape(1, width),
        scan_state.reshape(rows, width, STATE),
        output_weight,
    )

    experts = expert_gate.shape[0] * n_ep
    lanes = -(-experts // 128) * 128
    layer_out = pl.pallas_call(
        functools.partial(expert_kernel, n_ep, n_tp),
        out_shape=shape((rows, columns), BF16),
        in_specs=[vmem] * 5 + [hbm] * 6,
        out_specs=vmem,
        scratch_shapes=[
            pltpu.VMEM(expert_gate.shape, BF16),
            pltpu.VMEM(expert_up.shape, BF16),
            pltpu.VMEM(expert_down.shape, BF16),
            pltpu.VMEM(shared_gate.shape, BF16),
            pltpu.VMEM(shared_up.shape, BF16),
            pltpu.VMEM(shared_down.shape, BF16),
            pltpu.VMEM((n_tp, rows, columns), BF16),
            pltpu.VMEM((n_ep, n_tp, rows, columns), BF16),
            pltpu.VMEM((n_ep, rows, lanes), F32),
            pltpu.VMEM((n_ep * rows, model), BF16),
            pltpu.VMEM((n_tp, n_ep, rows, columns), F32),
            pltpu.VMEM((n_tp, n_ep, rows, columns), BF16),
            pltpu.VMEM((n_all, rows, columns), BF16),
            dma((6,)),
            dma((n_tp,)),
            dma((n_tp,)),
            dma((n_ep,)),
            dma((n_ep,)),
            dma((n_all,)),
            dma((n_all,)),
            dma((n_all,)),
            dma((n_all,)),
        ],
        compiler_params=pltpu.CompilerParams(
            collective_id=1, has_side_effects=True, vmem_limit_bytes=VMEM_LIMIT
        ),
        name="experts",
    )(
        part,
        tokens,
        routes,
        route_weight,
        channel_gain.reshape(1, model),
        expert_gate,
        expert_up,
        expert_down,
        shared_gate,
        shared_up,
        shared_down,
    )
    return (
        layer_out,
        new_state.reshape(scan_state.shape),
        jnp.transpose(new_filter, (1, 0, 2)),
    )


def solution(mesh):
    in_specs = (
        P("ep", None),
        P("ep", None),
        P("ep", None),
        P(),
        P(None, "tp"),
        P(None, "tp"),
        P(None, "tp"),
        P("tp", None),
        P("tp", None),
        P("tp"),
        P("tp"),
        P("ep", "tp"),
        P(None, "tp"),
        P("ep", None, "tp"),
        P("ep", "tp", None, None),
        P("tp"),
        P("tp"),
        P("tp", None),
        P(),
        P("ep", None, "tp"),
        P("ep", None, "tp"),
        P("ep", "tp", None),
        P(None, "tp"),
        P(None, "tp"),
        P("tp", None),
    )
    out_specs = (P("ep", "tp"), P("ep", "tp", None, None), P("ep", None, "tp"))
    return jax.shard_map(
        on_device, mesh=mesh, in_specs=in_specs, out_specs=out_specs, check_vma=False
    )
```

```python
import functools

import jax
import jax.numpy as jnp
from jax import lax
from jax.experimental import pallas as pl
from jax.experimental.pallas import tpu as pltpu
from jax.sharding import PartitionSpec as P

HEADS = 64
HEAD_DIM = 64
GROUPS = 4
STATE = 128

EPS = 1e-06
F32 = jnp.float32
BF16 = jnp.bfloat16
MESH = pl.DeviceIdType.MESH
VMEM_LIMIT = 56 * 1024 * 1024


def dot(a, b):
    return jnp.dot(a, b, preferred_element_type=F32)


def dot_nt(a, b):
    return lax.dot_general(a, b, (((1,), (1,)), ((), ())), preferred_element_type=F32)


def split(v):
    high = v.astype(BF16)
    return high, (v - high.astype(F32)).astype(BF16)


def softplus(v):
    return jnp.maximum(v, 0.0) + jnp.log1p(jnp.exp(-jnp.abs(v)))


def project_kernel(
    n_tp,
    heads_here,
    tokens_ref,
    gain_ref,
    step_ref,
    gate_hbm,
    input_hbm,
    write_hbm,
    read_hbm,
    vec_ref,
    gate_ref,
    input_ref,
    raw_ref,
    gate_buf,
    input_buf,
    write_buf,
    read_buf,
    normed_buf,
    out_buf,
    in_buf,
    load_sem,
    send_sem,
    recv_sem,
):
    ep = lax.axis_index("ep")
    tp = lax.axis_index("tp")
    loads = [
        pltpu.make_async_copy(src, dst, load_sem.at[i])
        for i, (src, dst) in enumerate(
            (
                (write_hbm, write_buf),
                (read_hbm, read_buf),
                (input_hbm, input_buf),
                (gate_hbm, gate_buf),
            )
        )
    ]
    for load in loads:
        load.start()
    barrier = pltpu.get_barrier_semaphore()

    def greet(k, carry):
        pl.semaphore_signal(
            barrier, inc=1, device_id=(ep, lax.rem(tp + k, n_tp)), device_id_type=MESH
        )
        return carry

    lax.fori_loop(1, n_tp, greet, 0)
    tokens = tokens_ref[...].astype(F32)
    scale = lax.rsqrt(jnp.mean(tokens * tokens, axis=-1, keepdims=True) + EPS)
    normed_buf[...] = (tokens * scale * gain_ref[...]).astype(BF16)
    features = write_buf.shape[0]
    own = normed_buf[:, pl.ds(pl.multiple_of(tp * features, features), features)]
    loads[0].wait()
    loads[1].wait()
    write_part = dot(own, write_buf[...]).astype(BF16)
    read_part = dot(own, read_buf[...]).astype(BF16)
    for g in range(GROUPS):
        out_buf[g, :, :STATE] = write_part[:, g * STATE : (g + 1) * STATE]
        out_buf[g, :, STATE:] = read_part[:, g * STATE : (g + 1) * STATE]
    per_group = HEADS // GROUPS
    pl.semaphore_wait(barrier, n_tp - 1)

    def copy_to(k):
        peer = lax.rem(tp + k, n_tp)
        return pltpu.make_async_remote_copy(
            src_ref=out_buf.at[(peer * heads_here) // per_group],
            dst_ref=in_buf.at[tp],
            send_sem=send_sem.at[peer],
            recv_sem=recv_sem.at[tp],
            device_id=(ep, peer),
            device_id_type=MESH,
        )

    def copy_from(k):
        peer = lax.rem(tp + k, n_tp)
        return pltpu.make_async_remote_copy(
            src_ref=out_buf.at[0],
            dst_ref=in_buf.at[peer],
            send_sem=send_sem.at[peer],
            recv_sem=recv_sem.at[peer],
            device_id=(ep, peer),
            device_id_type=MESH,
        )

    def send(k, carry):
        copy_to(k).start()
        return carry

    lax.fori_loop(1, n_tp, send, 0)
    in_buf[tp] = out_buf[(tp * heads_here) // per_group]
    normed = normed_buf[...]
    raw_ref[...] = dot_nt(step_ref[...], normed)
    loads[2].wait()
    input_ref[...] = dot(normed, input_buf[...]).astype(BF16)
    loads[3].wait()
    gate_ref[...] = dot(normed, gate_buf[...]).astype(BF16)

    def receive(k, carry):
        copy_from(k).wait_recv()
        return carry

    lax.fori_loop(1, n_tp, receive, 0)
    vec_ref[...] = jax.nn.silu(jnp.sum(in_buf[...].astype(F32), axis=0))

    def sent(k, carry):
        copy_to(k).wait_send()
        return carry

    lax.fori_loop(1, n_tp, sent, 0)


def state_kernel(
    bias_ref,
    rate_ref,
    skip_ref,
    vec_ref,
    gate_ref,
    input_ref,
    raw_ref,
    jolt_ref,
    taps_ref,
    filter_ref,
    gain_ref,
    state_hbm,
    weight_hbm,
    part_ref,
    new_hbm,
    new_filter_ref,
    state_buf,
    new_buf,
    weight_buf,
    decay_buf,
    x_buf,
    read_buf,
    load_sem,
    store_sem,
    weight_sem,
):
    rows, width, _ = state_buf.shape
    heads = jolt_ref.shape[0]
    for s in range(rows):
        pltpu.make_async_copy(state_hbm.at[s], state_buf.at[s], load_sem.at[s]).start()
    weight_load = pltpu.make_async_copy(weight_hbm, weight_buf, weight_sem)
    weight_load.start()
    taps = taps_ref[...].astype(F32)
    last = filter_ref.shape[0]
    inputs = input_ref[...]
    total = inputs.astype(F32) * taps[last : last + 1]
    for i in range(last):
        total = total + filter_ref[i].astype(F32) * taps[i : i + 1]
        new_filter_ref[i] = filter_ref[i + 1] if i + 1 < last else inputs
    filtered = jax.nn.silu(total)
    pad = jnp.zeros((128 - rows, width), F32)
    filtered_t = jnp.transpose(jnp.concatenate([filtered, pad], axis=0))[:, :rows]
    head_ids = lax.broadcasted_iota(jnp.int32, (heads, rows), 0)
    bias = jnp.zeros((heads, rows), F32)
    rate = jnp.zeros((heads, rows), F32)
    for h in range(heads):
        bias = jnp.where(head_ids == h, bias_ref[h], bias)
        rate = jnp.where(head_ids == h, rate_ref[h], rate)
    step = softplus(raw_ref[...] + bias)
    decay = jnp.exp(jolt_ref[...] - jnp.exp(rate) * step)

    def expand(v):
        return jnp.concatenate(
            [jnp.broadcast_to(v[h : h + 1], (HEAD_DIM, rows)) for h in range(heads)], axis=0
        )

    decay_buf[...] = expand(decay)
    x_buf[...] = expand(step) * filtered_t
    for s in range(rows):
        pltpu.make_async_copy(state_hbm.at[s], state_buf.at[s], load_sem.at[s]).wait()
        write = vec_ref[s : s + 1, :STATE]
        new = decay_buf[:, s : s + 1] * state_buf[s] + x_buf[:, s : s + 1] * write
        new_buf[s] = new
        pltpu.make_async_copy(new_buf.at[s], new_hbm.at[s], store_sem.at[s]).start()
        read_high, read_low = split(vec_ref[s : s + 1, STATE:])
        high, low = split(new)
        read_buf[s : s + 1, :] = (
            dot_nt(read_high, high) + dot_nt(read_low, high) + dot_nt(read_high, low)
        )
    lane_head = lax.broadcasted_iota(jnp.int32, (1, width), 1) // HEAD_DIM
    skip = jnp.zeros((1, width), F32)
    for h in range(heads):
        skip = jnp.where(lane_head == h, skip_ref[h], skip)
    value = (read_buf[...] + skip * filtered) * jax.nn.silu(gate_ref[...].astype(F32))
    same = (
        lax.broadcasted_iota(jnp.int32, (width, width), 0) // HEAD_DIM
        == lax.broadcasted_iota(jnp.int32, (width, width), 1) // HEAD_DIM
    )
    block = jnp.where(same, 1.0, 0.0).astype(BF16)
    high, low = split(value * value)
    mean_square = (dot(high, block) + dot(low, block)) * (1.0 / HEAD_DIM)
    gated = (value * lax.rsqrt(mean_square + EPS) * gain_ref[...]).astype(BF16)
    weight_load.wait()
    columns = part_ref.shape[2]
    for t in range(part_ref.shape[0]):
        part_ref[t] = dot(gated, weight_buf[:, t * columns : (t + 1) * columns]).astype(BF16)
    for s in range(rows):
        pltpu.make_async_copy(new_buf.at[s], new_hbm.at[s], store_sem.at[s]).wait()


def expert_kernel(
    n_ep,
    n_tp,
    part_ref,
    tokens_ref,
    routes_ref,
    route_weight_ref,
    gain_ref,
    gate_hbm,
    up_hbm,
    down_hbm,
    sgate_hbm,
    sup_hbm,
    sdown_hbm,
    out_ref,
    gate_buf,
    up_buf,
    down_buf,
    sgate_buf,
    sup_buf,
    sdown_buf,
    mix_buf,
    resid_buf,
    share_buf,
    normed_buf,
    total_buf,
    shared_buf,
    term_buf,
    back_buf,
    load_sem,
    mix_send,
    mix_recv,
    share_send,
    share_recv,
    resid_send,
    resid_recv,
    back_send,
    back_recv,
):
    ep = lax.axis_index("ep")
    tp = lax.axis_index("tp")
    me = ep * n_tp + tp
    n_all = n_ep * n_tp
    rows, columns = out_ref.shape
    loads = [
        pltpu.make_async_copy(src, dst, load_sem.at[i])
        for i, (src, dst) in enumerate(
            (
                (sgate_hbm, sgate_buf),
                (sup_hbm, sup_buf),
                (sdown_hbm, sdown_buf),
                (gate_hbm, gate_buf),
                (up_hbm, up_buf),
                (down_hbm, down_buf),
            )
        )
    ]
    barrier = pltpu.get_barrier_semaphore()

    def place(k):
        other = lax.rem(me + k, n_all)
        return other // n_tp, lax.rem(other, n_tp)

    def loop(low, high, act):
        def body(k, carry):
            act(k)
            return carry

        lax.fori_loop(low, high, body, 0)

    loop(
        1,
        n_all,
        lambda k: pl.semaphore_signal(barrier, inc=1, device_id=place(k), device_id_type=MESH),
    )
    for load in loads:
        load.start()

    lanes = share_buf.shape[2]
    ids = lax.broadcasted_iota(jnp.int32, (lanes, rows), 0)
    share = jnp.zeros((lanes, rows), F32)
    for k in range(routes_ref.shape[0]):
        share = share + jnp.where(
            routes_ref[k : k + 1, :] == ids, route_weight_ref[k : k + 1, :], 0.0
        )
    pad = jnp.zeros((lanes, 128 - rows), F32)
    share_buf[ep] = jnp.transpose(jnp.concatenate([share, pad], axis=1))[:rows]

    def mix_copy(k, slot):
        peer = lax.rem(tp + k, n_tp)
        return pltpu.make_async_remote_copy(
            src_ref=part_ref.at[peer],
            dst_ref=mix_buf.at[tp if slot is None else peer],
            send_sem=mix_send.at[peer],
            recv_sem=mix_recv.at[tp if slot is None else peer],
            device_id=(ep, peer),
            device_id_type=MESH,
        )

    def share_copy(k, slot):
        peer = lax.rem(ep + k, n_ep)
        mine = ep if slot is None else peer
        return pltpu.make_async_remote_copy(
            src_ref=share_buf.at[mine],
            dst_ref=share_buf.at[mine],
            send_sem=share_send.at[peer],
            recv_sem=share_recv.at[mine],
            device_id=(peer, tp),
            device_id_type=MESH,
        )

    def resid_copy(e, t, slot):
        at_e, at_t = (ep, tp) if slot is None else (e, t)
        return pltpu.make_async_remote_copy(
            src_ref=resid_buf.at[at_e, at_t],
            dst_ref=resid_buf.at[at_e, at_t],
            send_sem=resid_send.at[e * n_tp + t],
            recv_sem=resid_recv.at[at_e * n_tp + at_t],
            device_id=(e, t),
            device_id_type=MESH,
        )

    def back_copy(e, t, slot):
        at_e, at_t = (ep, tp) if slot is None else (e, t)
        return pltpu.make_async_remote_copy(
            src_ref=term_buf.at[t, e],
            dst_ref=back_buf.at[at_e * n_tp + at_t],
            send_sem=back_send.at[e * n_tp + t],
            recv_sem=back_recv.at[at_e * n_tp + at_t],
            device_id=(e, t),
            device_id_type=MESH,
        )

    pl.semaphore_wait(barrier, n_all - 1)
    loop(1, n_tp, lambda k: mix_copy(k, None).start())
    loop(1, n_ep, lambda k: share_copy(k, None).start())
    mix_buf[tp] = part_ref[tp]
    own_tokens = tokens_ref[:, pl.ds(pl.multiple_of(tp * columns, columns), columns)]
    loop(1, n_tp, lambda k: mix_copy(k, 1).wait_recv())
    mixed = jnp.sum(mix_buf[...].astype(F32), axis=0).astype(BF16)
    resid_own = (own_tokens.astype(F32) + mixed.astype(F32)).astype(BF16)
    resid_buf[ep, tp] = resid_own
    def own_group(act):
        loop(1, n_tp, lambda k: act(ep, lax.rem(tp + k, n_tp)))

    def other_groups(act):
        def body(k):
            act(lax.rem(ep + 1 + k // n_tp, n_ep), lax.rem(tp + lax.rem(k, n_tp), n_tp))

        loop(0, (n_ep - 1) * n_tp, body)

    own_group(lambda e, t: resid_copy(e, t, None).start())
    other_groups(lambda e, t: resid_copy(e, t, None).start())

    def normalise(e):
        square = jnp.zeros((rows, columns), F32)
        for t in range(n_tp):
            value = resid_buf[e, t].astype(F32)
            square = square + value * value
        mean_square = jnp.sum(square, axis=-1, keepdims=True) * (1.0 / (n_tp * columns))
        scale = lax.rsqrt(mean_square + EPS)
        for t in range(n_tp):
            at = slice(t * columns, (t + 1) * columns)
            value = resid_buf[e, t].astype(F32) * scale * gain_ref[:, at]
            normed_buf[pl.ds(pl.multiple_of(e * rows, rows), rows), at] = value.astype(BF16)

    own_group(lambda e, t: resid_copy(e, t, 1).wait_recv())
    normalise(ep)
    normed_own = normed_buf[pl.ds(pl.multiple_of(ep * rows, rows), rows), :]
    loads[0].wait()
    loads[1].wait()
    shared_hidden = (
        jax.nn.silu(dot(normed_own, sgate_buf[...])) * dot(normed_own, sup_buf[...])
    ).astype(BF16)
    loads[2].wait()
    for t in range(n_tp):
        at = slice(t * columns, (t + 1) * columns)
        shared_buf[t] = dot(shared_hidden, sdown_buf[:, at])
    other_groups(lambda e, t: resid_copy(e, t, 1).wait_recv())
    loop(1, n_ep, lambda k: normalise(lax.rem(ep + k, n_ep)))
    loads[3].wait()
    loads[4].wait()
    hidden = []
    for j in range(gate_buf.shape[0]):
        normed = normed_buf[...]
        hidden.append(
            (jax.nn.silu(dot(normed, gate_buf[j])) * dot(normed, up_buf[j])).astype(BF16)
        )
    loop(1, n_ep, lambda k: share_copy(k, 1).wait_recv())
    shares = share_buf[...].reshape(n_ep * rows, lanes)
    all_lanes = lax.broadcasted_iota(jnp.int32, shares.shape, 1)
    local = gate_buf.shape[0]
    scales = [
        jnp.sum(jnp.where(all_lanes == ep * local + j, shares, 0.0), axis=1, keepdims=True)
        for j in range(local)
    ]
    loads[5].wait()
    for t in range(n_tp):
        at = slice(t * columns, (t + 1) * columns)
        term = scales[0] * dot(hidden[0], down_buf[0, :, at])
        for j in range(1, local):
            term = term + scales[j] * dot(hidden[j], down_buf[j, :, at])
        total_buf[t] = term.reshape(n_ep, rows, columns)
        total_buf[t, ep] = total_buf[t, ep] + shared_buf[t]
        term_buf[t] = total_buf[t].astype(BF16)

        def give(e):
            @pl.when(e * n_tp + t != me)
            def _():
                back_copy(e, t, None).start()

        loop(0, n_ep, give)
    back_buf[me] = term_buf[tp, ep]

    def others(act):
        def body(k):
            e, t = place(k)
            act(e, t)

        loop(1, n_all, body)

    others(lambda e, t: back_copy(e, t, 1).wait_recv())
    out_ref[...] = (
        resid_buf[ep, tp].astype(F32) + jnp.sum(back_buf[...].astype(F32), axis=0)
    ).astype(BF16)
    loop(1, n_tp, lambda k: mix_copy(k, None).wait_send())
    loop(1, n_ep, lambda k: share_copy(k, None).wait_send())
    own_group(lambda e, t: resid_copy(e, t, None).wait_send())
    other_groups(lambda e, t: resid_copy(e, t, None).wait_send())
    others(lambda e, t: back_copy(e, t, None).wait_send())


def on_device(
    tokens,
    routes,
    route_weight,
    mixer_gain,
    gate_weight,
    input_weight,
    step_weight,
    write_weight,
    read_weight,
    step_bias,
    decay_log,
    decay_jolt,
    filter_taps,
    filter_state,
    scan_state,
    skip_gain,
    head_gain,
    output_weight,
    channel_gain,
    expert_gate,
    expert_up,
    expert_down,
    shared_gate,
    shared_up,
    shared_down,
):
    rows, model = tokens.shape
    n_tp = lax.axis_size("tp")
    n_ep = lax.axis_size("ep")
    n_all = n_tp * n_ep
    columns = model // n_tp
    heads_here = step_bias.shape[0]
    width = gate_weight.shape[1]
    vmem = pl.BlockSpec(memory_space=pltpu.VMEM)
    smem = pl.BlockSpec(memory_space=pltpu.SMEM)
    hbm = pl.BlockSpec(memory_space=pl.ANY)
    dma = pltpu.SemaphoreType.DMA
    shape = jax.ShapeDtypeStruct

    vecs, gate_rows, input_rows, step_raw = pl.pallas_call(
        functools.partial(project_kernel, n_tp, heads_here),
        out_shape=(
            shape((rows, 2 * STATE), F32),
            shape((rows, width), BF16),
            shape((rows, width), BF16),
            shape((heads_here, rows), F32),
        ),
        in_specs=[vmem] * 3 + [hbm] * 4,
        out_specs=(vmem,) * 4,
        scratch_shapes=[
            pltpu.VMEM(gate_weight.shape, BF16),
            pltpu.VMEM(input_weight.shape, BF16),
            pltpu.VMEM(write_weight.shape, BF16),
            pltpu.VMEM(read_weight.shape, BF16),
            pltpu.VMEM((rows, model), BF16),
            pltpu.VMEM((GROUPS, rows, 2 * STATE), BF16),
            pltpu.VMEM((n_tp, rows, 2 * STATE), BF16),
            dma((4,)),
            dma((n_tp,)),
            dma((n_tp,)),
        ],
        compiler_params=pltpu.CompilerParams(
            collective_id=0, has_side_effects=True, vmem_limit_bytes=VMEM_LIMIT
        ),
        name="project",
    )(
        tokens,
        mixer_gain.reshape(1, model),
        step_weight.T,
        gate_weight,
        input_weight,
        write_weight,
        read_weight,
    )

    taps = filter_state.shape[1]
    part, new_state, new_filter = pl.pallas_call(
        state_kernel,
        out_shape=(
            shape((n_tp, rows, columns), BF16),
            shape((rows, width, STATE), F32),
            shape((taps, rows, width), BF16),
        ),
        in_specs=[smem] * 3 + [vmem] * 8 + [hbm] * 2,
        out_specs=(vmem, hbm, vmem),
        scratch_shapes=[
            pltpu.VMEM((rows, width, STATE), F32),
            pltpu.VMEM((rows, width, STATE), F32),
            pltpu.VMEM(output_weight.shape, BF16),
            pltpu.VMEM((width, rows), F32),
            pltpu.VMEM((width, rows), F32),
            pltpu.VMEM((rows, width), F32),
            dma((rows,)),
            dma((rows,)),
            dma,
        ],
        compiler_params=pltpu.CompilerParams(vmem_limit_bytes=VMEM_LIMIT),
        name="state",
    )(
        step_bias,
        decay_log,
        skip_gain,
        vecs,
        gate_rows,
        input_rows,
        step_raw,
        decay_jolt.T,
        filter_taps,
        jnp.transpose(filter_state, (1, 0, 2)),
        head_gain.reshape(1, width),
        scan_state.reshape(rows, width, STATE),
        output_weight,
    )

    experts = expert_gate.shape[0] * n_ep
    lanes = -(-experts // 128) * 128
    layer_out = pl.pallas_call(
        functools.partial(expert_kernel, n_ep, n_tp),
        out_shape=shape((rows, columns), BF16),
        in_specs=[vmem] * 5 + [hbm] * 6,
        out_specs=vmem,
        scratch_shapes=[
            pltpu.VMEM(expert_gate.shape, BF16),
            pltpu.VMEM(expert_up.shape, BF16),
            pltpu.VMEM(expert_down.shape, BF16),
            pltpu.VMEM(shared_gate.shape, BF16),
            pltpu.VMEM(shared_up.shape, BF16),
            pltpu.VMEM(shared_down.shape, BF16),
            pltpu.VMEM((n_tp, rows, columns), BF16),
            pltpu.VMEM((n_ep, n_tp, rows, columns), BF16),
            pltpu.VMEM((n_ep, rows, lanes), F32),
            pltpu.VMEM((n_ep * rows, model), BF16),
            pltpu.VMEM((n_tp, n_ep, rows, columns), F32),
            pltpu.VMEM((n_tp, rows, columns), F32),
            pltpu.VMEM((n_tp, n_ep, rows, columns), BF16),
            pltpu.VMEM((n_all, rows, columns), BF16),
            dma((6,)),
            dma((n_tp,)),
            dma((n_tp,)),
            dma((n_ep,)),
            dma((n_ep,)),
            dma((n_all,)),
            dma((n_all,)),
            dma((n_all,)),
            dma((n_all,)),
        ],
        compiler_params=pltpu.CompilerParams(
            collective_id=1, has_side_effects=True, vmem_limit_bytes=VMEM_LIMIT
        ),
        name="experts",
    )(
        part,
        tokens,
        routes.T,
        route_weight.T,
        channel_gain.reshape(1, model),
        expert_gate,
        expert_up,
        expert_down,
        shared_gate,
        shared_up,
        shared_down,
    )
    return (
        layer_out,
        new_state.reshape(scan_state.shape),
        jnp.transpose(new_filter, (1, 0, 2)),
    )


def solution(mesh):
    in_specs = (
        P("ep", None),
        P("ep", None),
        P("ep", None),
        P(),
        P(None, "tp"),
        P(None, "tp"),
        P(None, "tp"),
        P("tp", None),
        P("tp", None),
        P("tp"),
        P("tp"),
        P("ep", "tp"),
        P(None, "tp"),
        P("ep", None, "tp"),
        P("ep", "tp", None, None),
        P("tp"),
        P("tp"),
        P("tp", None),
        P(),
        P("ep", None, "tp"),
        P("ep", None, "tp"),
        P("ep", "tp", None),
        P(None, "tp"),
        P(None, "tp"),
        P("tp", None),
    )
    out_specs = (P("ep", "tp"), P("ep", "tp", None, None), P("ep", None, "tp"))
    return jax.shard_map(
        on_device, mesh=mesh, in_specs=in_specs, out_specs=out_specs, check_vma=False
    )
```
